32 devices in a mesh: sp: 8 (over z, x), tp: 4 (over y, core).
Axes of the slice: x: 2, y: 2, z: 4, core: 2. Of those that a mesh axis runs over, the one named last changes fastest.
Arguments:
- tokens: bfloat16 [4096, 4096], P(('sp', 'tp')), may hold values from -6 to 6
- lock_projector: bfloat16 [4096, 1024], P(None, 'tp'), may hold values from -0.01171875 to 0.01171875
- value_weight: bfloat16 [4096, 2048], P(None, 'tp'), may hold values from -0.0234375 to 0.0234375
- decay_weight: bfloat16 [4096, 1024], P(None, 'tp'), may hold values from -0.09375 to 0.09375
- decay_offset: float32 [1024], P('tp'), may hold values from -3.5 to 0
- fresh_question: bfloat16 [16, 64], P('tp'), may hold values from -6 to 6
Outputs:
- state_cache: bfloat16 [16, 64, 128], P('tp', 'sp')
- first_read: bfloat16 [16, 128], P('tp')
The draws below stay inside these ranges and needn't reach their ends.
All inputs are finite; a program needn't handle non-finite values.
Results may differ from the reference program's by a relative error of at most 0.0034.
Values may be sent and summed in bfloat16 or wider, within the bound.
A program may use at most 64 MiB of HBM per device.

```python
import math
import jax
import jax.numpy as jnp
from jax import lax

D = 4096
H = 16
CUE_WIDTH = 64
DV = 128
PROMPT_SPAN = 4096


def block_levels(key, extent, pieces, low, high):
    factor_of = 1.0
    for position, blocks in pieces:
        heights = jax.random.uniform(jax.random.fold_in(jax.random.fold_in(key, 6), position), (blocks,), jnp.float32, low / len(pieces), high / len(pieces))
        factor_of = factor_of * jnp.repeat(jnp.exp(heights), extent[position] // blocks).reshape((-1,) + (1,) * (len(extent) - 1 - position))
    return factor_of


def noise(key, dims, scale, limit, shards=(), dtype=jnp.bfloat16):
    entries = scale * jax.random.normal(key, dims, jnp.float32)
    if shards:
        entries = entries * block_levels(key, dims, shards, -0.22, 0.18)
    return jnp.clip(entries, -limit, limit).astype(dtype)


def setup_inputs(seed: int = 0) -> dict:
    key_of = jax.random.split(jax.random.key(seed), 7)
    tokens = noise(key_of[0], (PROMPT_SPAN, D), 1.0, 6.0, ((0, 32),))
    lock_projector = noise(key_of[1], (D, H * CUE_WIDTH), (D * CUE_WIDTH) ** -0.5, 0.01171875, ((1, 4),))
    value_weight = noise(key_of[2], (D, H * DV), (D * 16) ** -0.5, 0.0234375, ((1, 4),))
    decay_weight = noise(key_of[3], (D, H * CUE_WIDTH), D ** -0.5, 0.09375, ((1, 4),))
    decay_offset = jnp.clip(-3.5 + 3.5 * jax.random.uniform(key_of[4], (H * CUE_WIDTH,), jnp.float32) ** block_levels(key_of[4], (H * CUE_WIDTH,), ((0, 4),), -0.2, 0.2), -3.5, 0.0)
    fresh_question = noise(key_of[5], (H, CUE_WIDTH), 1.0, 6.0, ((0, 4),))
    return dict(tokens=tokens, lock_projector=lock_projector, value_weight=value_weight, decay_weight=decay_weight, decay_offset=decay_offset, fresh_question=fresh_question)


decay_tau = 16.0

def reference(tokens, lock_projector, value_weight, decay_weight, decay_offset, fresh_question):
    lock_vectors = jnp.dot(tokens, lock_projector, preferred_element_type=jnp.float32).astype(jnp.bfloat16)
    value_rows = jnp.dot(tokens, value_weight, preferred_element_type=jnp.float32).astype(jnp.bfloat16)
    decay_pre = jnp.dot(tokens, decay_weight, preferred_element_type=jnp.float32)
    log_decay = jax.nn.log_sigmoid(decay_pre + decay_offset[None, :] + math.log(PROMPT_SPAN)) / decay_tau
    totals = lax.optimization_barrier(jnp.sum(log_decay, axis=0))
    after = totals[None, :] - jnp.cumsum(log_decay, axis=0)
    weighted = (lock_vectors.astype(jnp.float32) * jnp.exp(after)).astype(jnp.bfloat16)
    lookup_probes = weighted.astype(jnp.float32).reshape(PROMPT_SPAN, H, CUE_WIDTH)
    stored_contents = value_rows.astype(jnp.float32).reshape(PROMPT_SPAN, H, DV)
    recall_grid = jnp.einsum('nyl,nyp->ylp', lookup_probes, stored_contents)
    attended_blend = CUE_WIDTH ** (-0.5) * jnp.einsum('qw,qwi->qi', fresh_question.astype(jnp.float32), recall_grid, precision=lax.Precision.HIGHEST)
    first_read = attended_blend * lax.rsqrt(lax.optimization_barrier(jnp.mean(attended_blend * attended_blend, axis=-1, keepdims=True)) + 1.0)
    return (recall_grid.astype(jnp.bfloat16), first_read.astype(jnp.bfloat16))
```

```python
import functools
import math

import jax
import jax.numpy as jnp
from jax import lax
from jax.experimental import pallas as pl
from jax.experimental.pallas import tpu as pltpu
from jax.sharding import PartitionSpec as P

DECAY_TAU = 16.0
CORES = 2
LANES = 128
MESH = pl.DeviceIdType.MESH


def kernel(
    n_sp, n_tp, chunks,
    tokens, w_key, w_value, w_decay, offset, question,
    cache_out, read_out,
    x_buf, key_buf, value_buf, decay_buf, key_acc, value_acc, decay_acc,
    log_buf, pair_total, spread_q, total_send, total_recv, state_send, state_recv,
    token_sem, weight_sem, y_send, y_recv, d_send, d_recv, t_send, t_recv, s_send, s_recv,
):
    rows, width = tokens.shape
    key_cols = w_key.shape[1]
    heads, cue = question.shape
    dv = w_value.shape[1] // heads
    depth = width // chunks
    pairs = n_tp // CORES
    pair_rows = CORES * rows
    row_span = cue // n_sp
    lanes_padded = total_send.shape[-1]
    length = rows * n_tp * n_sp

    sp = lax.axis_index("sp")
    tp = lax.axis_index("tp")
    pair = tp // CORES
    core = lax.rem(tp, CORES)
    partner = pair * CORES + (1 - core)

    def pair_at(i):
        return lax.rem(pair + pairs - i, pairs)

    def token_copy(c):
        start = c * depth if isinstance(c, int) else pl.multiple_of(c * depth, depth)
        return pltpu.make_async_copy(
            tokens.at[:, pl.ds(start, depth)], x_buf.at[c, pair, core], token_sem.at[c]
        )

    def weight_copies(c):
        start = c * depth if isinstance(c, int) else pl.multiple_of(c * depth, depth)
        return [
            pltpu.make_async_copy(w.at[pl.ds(start, depth), :], b.at[c], weight_sem.at[n, c])
            for n, (w, b) in enumerate(
                ((w_decay, decay_buf), (w_key, key_buf), (w_value, value_buf))
            )
        ]

    def across_send(i, c):
        to = lax.rem(pair + i, pairs) * CORES + core
        block = x_buf.at[c, pair, core]
        return pltpu.make_async_remote_copy(
            block, block, y_send.at[i, c], y_recv.at[i, c], device_id={"tp": to}, device_id_type=MESH
        )

    def across_recv(i, c):
        block = x_buf.at[c, pair_at(i), core]
        return pltpu.make_async_remote_copy(
            block, block, y_send.at[i, c], y_recv.at[i, c],
            device_id={"tp": pair_at(i) * CORES + core}, device_id_type=MESH,
        )

    def beside(i, c, which):
        block = x_buf.at[c, pair_at(i), which]
        return pltpu.make_async_remote_copy(
            block, block, d_send.at[i, c], d_recv.at[i, c],
            device_id={"tp": partner}, device_id_type=MESH,
        )

    def total_copy(i, slot):
        return pltpu.make_async_remote_copy(
            total_send, total_recv.at[slot], t_send.at[i], t_recv.at[i],
            device_id={"sp": lax.rem(sp + i, n_sp)}, device_id_type=MESH,
        )

    def state_copy(i, slot):
        to = lax.rem(sp + i, n_sp)
        return pltpu.make_async_remote_copy(
            state_send.at[to], state_recv.at[slot], s_send.at[i], s_recv.at[i],
            device_id={"sp": to}, device_id_type=MESH,
        )

    for c in range(chunks):
        token_copy(c).start()
    for c in range(chunks):
        for copy in weight_copies(c):
            copy.start()

    barrier = pltpu.get_barrier_semaphore()
    pl.semaphore_signal(barrier, inc=1, device_id={"tp": partner}, device_id_type=MESH)
    for i in range(1, pairs):
        pl.semaphore_signal(
            barrier, inc=1,
            device_id={"tp": lax.rem(pair + i, pairs) * CORES + core}, device_id_type=MESH,
        )
    for i in range(1, n_sp):
        pl.semaphore_signal(
            barrier, inc=1, device_id={"sp": lax.rem(sp + i, n_sp)}, device_id_type=MESH
        )

    wide_q = question[...].astype(jnp.float32)
    eye = lax.broadcasted_iota(jnp.int32, (cue, cue), 0) == lax.broadcasted_iota(
        jnp.int32, (cue, cue), 1
    )
    ones = jnp.ones((cue, dv), jnp.bfloat16)
    for h in range(heads):
        diagonal = jnp.where(eye, jnp.broadcast_to(wide_q[h : h + 1, :], (cue, cue)), 0.0)
        spread_q[h] = jnp.dot(
            diagonal.astype(jnp.bfloat16), ones, preferred_element_type=jnp.float32
        )

    pl.semaphore_wait(barrier, 1 + (pairs - 1) + (n_sp - 1))

    for c in range(chunks):
        token_copy(c).wait()
        for i in range(1, pairs):
            across_send(i, c).start()
        beside(0, c, core).start()

    def product(p, c, buf, acc, first):
        x = x_buf[c, p].reshape(pair_rows, depth)
        out = jnp.dot(x, buf[c], preferred_element_type=jnp.float32)
        if first:
            acc[p] = out
        else:
            acc[p] += out

    def all_products(p, c, first):
        product(p, c, decay_buf, decay_acc, first)
        product(p, c, key_buf, key_acc, first)
        product(p, c, value_buf, value_acc, first)

    def finish_decay(p):
        pre = decay_acc[p] + offset[...] + math.log(length)
        log_decay = (jnp.minimum(pre, 0.0) - jnp.log1p(jnp.exp(-jnp.abs(pre)))) / DECAY_TAU
        log_buf[p] = log_decay
        pair_total[p] = jnp.sum(log_decay, axis=0, keepdims=True)

    def send_totals():
        whole = pair_total[0]
        for p in range(1, pairs):
            whole = whole + pair_total[p]
        if lanes_padded > key_cols:
            whole = jnp.concatenate(
                [whole, jnp.zeros((1, lanes_padded - key_cols), jnp.float32)], axis=1
            )
        total_send[...] = whole
        total_recv[sp] = whole
        for i in range(1, n_sp):
            total_copy(i, sp).start()

    def arrive(i, c):
        if i == 0:
            for copy in weight_copies(c):
                copy.wait()
        else:
            across_recv(i, c).wait_recv()
            beside(i, c, core).start()

    for i in range(pairs):
        p = pair_at(i)
        arrive(i, 0)
        arrive(i, 1)
        beside(i, 0, 1 - core).wait_recv()
        all_products(p, 0, True)

        def step(c, carry, i=i, p=p):
            arrive(i, c + 1)
            beside(i, c, 1 - core).wait_recv()
            all_products(p, c, False)
            return carry

        lax.fori_loop(1, chunks - 1, step, 0)
        last = chunks - 1
        beside(i, last, 1 - core).wait_recv()
        product(p, last, decay_buf, decay_acc, False)
        finish_decay(p)
        if i == pairs - 1:
            send_totals()
        product(p, last, key_buf, key_acc, False)
        product(p, last, value_buf, value_acc, False)

    later = lax.broadcasted_iota(jnp.int32, (pair_rows, pair_rows), 1) > lax.broadcasted_iota(
        jnp.int32, (pair_rows, pair_rows), 0
    )
    later = jnp.where(later, 1.0, 0.0).astype(jnp.bfloat16)
    group = 2 if heads % 2 == 0 else 1
    gk, gv = group * cue, group * dv
    sums = [None] * (heads // group)
    behind = jnp.zeros((1, key_cols), jnp.float32)
    for p in reversed(range(pairs)):
        log_decay = log_buf[p]
        after = behind
        rest = log_decay
        for _ in range(3):
            part = rest.astype(jnp.bfloat16)
            rest = rest - part.astype(jnp.float32)
            after = after + jnp.dot(later, part, preferred_element_type=jnp.float32)
        behind = behind + pair_total[p]
        keys = key_acc[p].astype(jnp.bfloat16).astype(jnp.float32)
        weighted = (keys * jnp.exp(after)).astype(jnp.bfloat16)
        values = value_acc[p].astype(jnp.bfloat16)
        for g in range(heads // group):
            term = lax.dot_general(
                weighted[:, g * gk : (g + 1) * gk],
                values[:, g * gv : (g + 1) * gv],
                (((0,), (0,)), ((), ())),
                preferred_element_type=jnp.float32,
            )
            sums[g] = term if sums[g] is None else sums[g] + term

    for i in range(1, n_sp):
        total_copy(i, lax.rem(sp + n_sp - i, n_sp)).wait_recv()
    later_total = jnp.zeros((1, lanes_padded), jnp.float32)
    for s in range(n_sp):
        later_total = later_total + jnp.where(sp < s, total_recv[s], 0.0)
    kept = jnp.exp(later_total)
    base = heads * row_span
    for g in range(heads // group):
        lo = g * gk // LANES * LANES
        turned = jnp.broadcast_to(kept[:, lo : lo + LANES], (LANES, LANES)).T
        for j in range(group):
            h = g * group + j
            at = h * cue - lo
            spread = turned[at : at + cue]
            if dv != LANES:
                spread = jnp.broadcast_to(spread[:, :1], (cue, dv))
            state = sums[g][j * cue : (j + 1) * cue, j * dv : (j + 1) * dv] * spread
            heard = jnp.sum(state * spread_q[h], axis=0, keepdims=True) * cue**-0.5
            for s in range(n_sp):
                state_send[s, h * row_span : (h + 1) * row_span, :] = state[
                    s * row_span : (s + 1) * row_span
                ]
                state_send[s, base + h : base + h + 1, :] = heard
    for i in range(1, n_sp):
        state_copy(i, sp).start()
    state_recv[sp] = state_send[sp]
    for i in range(1, n_sp):
        state_copy(i, lax.rem(sp + n_sp - i, n_sp)).wait_recv()
    total = state_recv[0]
    for s in range(1, n_sp):
        total = total + state_recv[s]
    for h in range(heads):
        cache_out[h] = total[h * row_span : (h + 1) * row_span].astype(jnp.bfloat16)
    heard = total[base : base + heads]
    scale = lax.rsqrt(jnp.mean(heard * heard, axis=-1, keepdims=True) + 1.0)
    read_out[...] = (heard * scale).astype(jnp.bfloat16)

    def drain(c, carry):
        for i in range(1, pairs):
            across_send(i, c).wait_send()
        for i in range(pairs):
            beside(i, c, core).wait_send()
        return carry

    lax.fori_loop(0, chunks, drain, 0)
    for i in range(1, n_sp):
        total_copy(i, sp).wait_send()
        state_copy(i, sp).wait_send()


def per_device(n_sp, n_tp, tokens, lock_projector, value_weight, decay_weight, decay_offset, fresh_question):
    rows, width = tokens.shape
    key_cols = lock_projector.shape[1]
    value_cols = value_weight.shape[1]
    heads, cue = fresh_question.shape
    dv = value_cols // heads
    row_span = cue // n_sp
    pairs = n_tp // CORES
    chunks = 8
    depth = width // chunks
    lanes_padded = max(key_cols, LANES)
    message = -(-(heads * row_span + heads) // 8) * 8
    f32, bf16 = jnp.float32, jnp.bfloat16
    dma = pltpu.SemaphoreType.DMA
    any_spec = pl.BlockSpec(memory_space=pl.ANY)
    vmem_spec = pl.BlockSpec(memory_space=pltpu.VMEM)
    pair_rows = CORES * rows
    return pl.pallas_call(
        functools.partial(kernel, n_sp, n_tp, chunks),
        out_shape=(
            jax.ShapeDtypeStruct((heads, row_span, dv), bf16),
            jax.ShapeDtypeStruct((heads, dv), bf16),
        ),
        in_specs=[any_spec] * 4 + [vmem_spec] * 2,
        out_specs=(vmem_spec, vmem_spec),
        scratch_shapes=[
            pltpu.VMEM((chunks, pairs, CORES, rows, depth), bf16),
            pltpu.VMEM((chunks, depth, key_cols), bf16),
            pltpu.VMEM((chunks, depth, value_cols), bf16),
            pltpu.VMEM((chunks, depth, key_cols), bf16),
            pltpu.VMEM((pairs, pair_rows, key_cols), f32),
            pltpu.VMEM((pairs, pair_rows, value_cols), f32),
            pltpu.VMEM((pairs, pair_rows, key_cols), f32),
            pltpu.VMEM((pairs, pair_rows, key_cols), f32),
            pltpu.VMEM((pairs, 1, key_cols), f32),
            pltpu.VMEM((heads, cue, dv), f32),
            pltpu.VMEM((1, lanes_padded), f32),
            pltpu.VMEM((n_sp, 1, lanes_padded), f32),
            pltpu.VMEM((n_sp, message, dv), f32),
            pltpu.VMEM((n_sp, message, dv), f32),
            dma((chunks,)),
            dma((3, chunks)),
            dma((pairs, chunks)),
            dma((pairs, chunks)),
            dma((pairs, chunks)),
            dma((pairs, chunks)),
            dma((n_sp,)),
            dma((n_sp,)),
            dma((n_sp,)),
            dma((n_sp,)),
        ],
        compiler_params=pltpu.CompilerParams(
            collective_id=0, has_side_effects=True, vmem_limit_bytes=60 * 1024 * 1024
        ),
        name="gated_state",
    )(
        tokens, lock_projector, value_weight, decay_weight,
        decay_offset.reshape(1, key_cols), fresh_question,
    )


def solution(mesh):
    in_specs = (
        P(("sp", "tp"), None),
        P(None, "tp"),
        P(None, "tp"),
        P(None, "tp"),
        P("tp"),
        P("tp", None),
    )
    out_specs = (P("tp", "sp", None), P("tp", None))
    body = functools.partial(per_device, mesh.shape["sp"], mesh.shape["tp"])
    return jax.shard_map(body, mesh=mesh, in_specs=in_specs, out_specs=out_specs, check_vma=False)
```

```python
import functools
import math

import jax
import jax.numpy as jnp
from jax import lax
from jax.experimental import pallas as pl
from jax.experimental.pallas import tpu as pltpu
from jax.sharding import PartitionSpec as P

DECAY_TAU = 16.0
CORES = 2
LANES = 128
MESH = pl.DeviceIdType.MESH


def kernel(
    n_sp, n_tp, chunks,
    tokens, w_key, w_value, w_decay, offset, question,
    total_out,
    x_buf, key_buf, value_buf, decay_buf, key_acc, value_acc, decay_acc,
    log_buf, pair_total, spread_q, total_send, total_recv, state_send, state_recv,
    token_sem, weight_sem, y_send, y_recv, d_send, d_recv, t_send, t_recv, s_send, s_recv,
):
    rows, width = tokens.shape
    key_cols = w_key.shape[1]
    heads, cue = question.shape
    dv = w_value.shape[1] // heads
    depth = width // chunks
    pairs = n_tp // CORES
    pair_rows = CORES * rows
    row_span = cue // n_sp
    lanes_padded = total_send.shape[-1]
    length = rows * n_tp * n_sp

    sp = lax.axis_index("sp")
    tp = lax.axis_index("tp")
    pair = tp // CORES
    core = lax.rem(tp, CORES)
    partner = pair * CORES + (1 - core)

    def pair_at(i):
        return lax.rem(pair + pairs - i, pairs)

    def token_copy(c):
        start = c * depth if isinstance(c, int) else pl.multiple_of(c * depth, depth)
        return pltpu.make_async_copy(
            tokens.at[:, pl.ds(start, depth)], x_buf.at[c, pair, core], token_sem.at[c]
        )

    def weight_copies(c):
        start = c * depth if isinstance(c, int) else pl.multiple_of(c * depth, depth)
        return [
            pltpu.make_async_copy(w.at[pl.ds(start, depth), :], b.at[c], weight_sem.at[n, c])
            for n, (w, b) in enumerate(
                ((w_decay, decay_buf), (w_key, key_buf), (w_value, value_buf))
            )
        ]

    def across_send(i, c):
        to = lax.rem(pair + i, pairs) * CORES + core
        block = x_buf.at[c, pair, core]
        return pltpu.make_async_remote_copy(
            block, block, y_send.at[i, c], y_recv.at[i, c], device_id={"tp": to}, device_id_type=MESH
        )

    def across_recv(i, c):
        block = x_buf.at[c, pair_at(i), core]
        return pltpu.make_async_remote_copy(
            block, block, y_send.at[i, c], y_recv.at[i, c],
            device_id={"tp": pair_at(i) * CORES + core}, device_id_type=MESH,
        )

    def beside(i, c, which):
        block = x_buf.at[c, pair_at(i), which]
        return pltpu.make_async_remote_copy(
            block, block, d_send.at[i, c], d_recv.at[i, c],
            device_id={"tp": partner}, device_id_type=MESH,
        )

    def total_copy(i, slot):
        return pltpu.make_async_remote_copy(
            total_send, total_recv.at[slot], t_send.at[i], t_recv.at[i],
            device_id={"sp": lax.rem(sp + i, n_sp)}, device_id_type=MESH,
        )

    def state_copy(i, slot):
        to = lax.rem(sp + i, n_sp)
        return pltpu.make_async_remote_copy(
            state_send.at[to], state_recv.at[slot], s_send.at[i], s_recv.at[i],
            device_id={"sp": to}, device_id_type=MESH,
        )

    for c in range(chunks):
        token_copy(c).start()
    for c in range(chunks):
        for copy in weight_copies(c):
            copy.start()

    barrier = pltpu.get_barrier_semaphore()
    pl.semaphore_signal(barrier, inc=1, device_id={"tp": partner}, device_id_type=MESH)
    for i in range(1, pairs):
        pl.semaphore_signal(
            barrier, inc=1,
            device_id={"tp": lax.rem(pair + i, pairs) * CORES + core}, device_id_type=MESH,
        )
    for i in range(1, n_sp):
        pl.semaphore_signal(
            barrier, inc=1, device_id={"sp": lax.rem(sp + i, n_sp)}, device_id_type=MESH
        )

    wide_q = question[...].astype(jnp.float32)
    eye = lax.broadcasted_iota(jnp.int32, (cue, cue), 0) == lax.broadcasted_iota(
        jnp.int32, (cue, cue), 1
    )
    ones = jnp.ones((cue, dv), jnp.bfloat16)
    for h in range(heads):
        diagonal = jnp.where(eye, jnp.broadcast_to(wide_q[h : h + 1, :], (cue, cue)), 0.0)
        spread_q[h] = jnp.dot(
            diagonal.astype(jnp.bfloat16), ones, preferred_element_type=jnp.float32
        )

    pl.semaphore_wait(barrier, 1 + (pairs - 1) + (n_sp - 1))

    for c in range(chunks):
        token_copy(c).wait()
        for i in range(1, pairs):
            across_send(i, c).start()
        beside(0, c, core).start()

    def product(p, c, buf, acc, first):
        x = x_buf[c, p].reshape(pair_rows, depth)
        out = jnp.dot(x, buf[c], preferred_element_type=jnp.float32)
        if first:
            acc[p] = out
        else:
            acc[p] += out

    def all_products(p, c, first):
        product(p, c, decay_buf, decay_acc, first)
        product(p, c, key_buf, key_acc, first)
        product(p, c, value_buf, value_acc, first)

    def finish_decay(p):
        pre = decay_acc[p] + offset[...] + math.log(length)
        log_decay = (jnp.minimum(pre, 0.0) - jnp.log1p(jnp.exp(-jnp.abs(pre)))) / DECAY_TAU
        log_buf[p] = log_decay
        pair_total[p] = jnp.sum(log_decay, axis=0, keepdims=True)

    def send_totals():
        whole = pair_total[0]
        for p in range(1, pairs):
            whole = whole + pair_total[p]
        if lanes_padded > key_cols:
            whole = jnp.concatenate(
                [whole, jnp.zeros((1, lanes_padded - key_cols), jnp.float32)], axis=1
            )
        total_send[...] = whole
        total_recv[sp] = whole
        for i in range(1, n_sp):
            total_copy(i, sp).start()

    def arrive(i, c):
        if i == 0:
            for copy in weight_copies(c):
                copy.wait()
        else:
            across_recv(i, c).wait_recv()
            beside(i, c, core).start()

    for i in range(pairs):
        p = pair_at(i)
        arrive(i, 0)
        arrive(i, 1)
        beside(i, 0, 1 - core).wait_recv()
        all_products(p, 0, True)

        def step(c, carry, i=i, p=p):
            arrive(i, c + 1)
            beside(i, c, 1 - core).wait_recv()
            all_products(p, c, False)
            return carry

        lax.fori_loop(1, chunks - 1, step, 0)
        last = chunks - 1
        beside(i, last, 1 - core).wait_recv()
        product(p, last, decay_buf, decay_acc, False)
        finish_decay(p)
        if i == pairs - 1:
            send_totals()
        product(p, last, key_buf, key_acc, False)
        product(p, last, value_buf, value_acc, False)

    later = lax.broadcasted_iota(jnp.int32, (pair_rows, pair_rows), 1) > lax.broadcasted_iota(
        jnp.int32, (pair_rows, pair_rows), 0
    )
    later = jnp.where(later, 1.0, 0.0).astype(jnp.bfloat16)
    group = 2 if heads % 2 == 0 else 1
    gk, gv = group * cue, group * dv
    sums = [None] * (heads // group)
    behind = jnp.zeros((1, key_cols), jnp.float32)
    for p in reversed(range(pairs)):
        log_decay = log_buf[p]
        after = behind
        rest = log_decay
        for _ in range(3):
            part = rest.astype(jnp.bfloat16)
            rest = rest - part.astype(jnp.float32)
            after = after + jnp.dot(later, part, preferred_element_type=jnp.float32)
        behind = behind + pair_total[p]
        keys = key_acc[p].astype(jnp.bfloat16).astype(jnp.float32)
        exact = keys * jnp.exp(after)
        upper = exact.astype(jnp.bfloat16)
        lower = (exact - upper.astype(jnp.float32)).astype(jnp.bfloat16)
        values = value_acc[p].astype(jnp.bfloat16)
        for g in range(heads // group):
            for weighted in (upper, lower):
                term = lax.dot_general(
                    weighted[:, g * gk : (g + 1) * gk],
                    values[:, g * gv : (g + 1) * gv],
                    (((0,), (0,)), ((), ())),
                    preferred_element_type=jnp.float32,
                )
                sums[g] = term if sums[g] is None else sums[g] + term

    for i in range(1, n_sp):
        total_copy(i, lax.rem(sp + n_sp - i, n_sp)).wait_recv()
    later_total = jnp.zeros((1, lanes_padded), jnp.float32)
    for s in range(n_sp):
        later_total = later_total + jnp.where(sp < s, total_recv[s], 0.0)
    kept = jnp.exp(later_total)
    base = heads * row_span
    for g in range(heads // group):
        lo = g * gk // LANES * LANES
        turned = jnp.broadcast_to(kept[:, lo : lo + LANES], (LANES, LANES)).T
        for j in range(group):
            h = g * group + j
            at = h * cue - lo
            spread = turned[at : at + cue]
            if dv != LANES:
                spread = jnp.broadcast_to(spread[:, :1], (cue, dv))
            state = sums[g][j * cue : (j + 1) * cue, j * dv : (j + 1) * dv] * spread
            heard = jnp.sum(state * spread_q[h], axis=0, keepdims=True) * cue**-0.5
            for s in range(n_sp):
                state_send[s, h * row_span : (h + 1) * row_span, :] = state[
                    s * row_span : (s + 1) * row_span
                ]
                state_send[s, base + h : base + h + 1, :] = heard
    for i in range(1, n_sp):
        state_copy(i, sp).start()
    state_recv[sp] = state_send[sp]
    for i in range(1, n_sp):
        state_copy(i, lax.rem(sp + n_sp - i, n_sp)).wait_recv()
    total = state_recv[0]
    for s in range(1, n_sp):
        total = total + state_recv[s]
    total_out[...] = total

    def drain(c, carry):
        for i in range(1, pairs):
            across_send(i, c).wait_send()
        for i in range(pairs):
            beside(i, c, core).wait_send()
        return carry

    lax.fori_loop(0, chunks, drain, 0)
    for i in range(1, n_sp):
        total_copy(i, sp).wait_send()
        state_copy(i, sp).wait_send()


def finish(heads, row_span, total, cache_out, read_out):
    for h in range(heads):
        cache_out[h] = total[h * row_span : (h + 1) * row_span, :].astype(jnp.bfloat16)
    heard = total[heads * row_span : heads * (row_span + 1), :]
    scale = lax.rsqrt(jnp.mean(heard * heard, axis=-1, keepdims=True) + 1.0)
    read_out[...] = (heard * scale).astype(jnp.bfloat16)


def per_device(n_sp, n_tp, tokens, lock_projector, value_weight, decay_weight, decay_offset, fresh_question):
    rows, width = tokens.shape
    key_cols = lock_projector.shape[1]
    value_cols = value_weight.shape[1]
    heads, cue = fresh_question.shape
    dv = value_cols // heads
    row_span = cue // n_sp
    pairs = n_tp // CORES
    chunks = 8
    depth = width // chunks
    lanes_padded = max(key_cols, LANES)
    message = -(-(heads * row_span + heads) // 8) * 8
    f32, bf16 = jnp.float32, jnp.bfloat16
    dma = pltpu.SemaphoreType.DMA
    any_spec = pl.BlockSpec(memory_space=pl.ANY)
    vmem_spec = pl.BlockSpec(memory_space=pltpu.VMEM)
    pair_rows = CORES * rows
    total = pl.pallas_call(
        functools.partial(kernel, n_sp, n_tp, chunks),
        out_shape=jax.ShapeDtypeStruct((message, dv), f32),
        in_specs=[any_spec] * 4 + [vmem_spec] * 2,
        out_specs=vmem_spec,
        scratch_shapes=[
            pltpu.VMEM((chunks, pairs, CORES, rows, depth), bf16),
            pltpu.VMEM((chunks, depth, key_cols), bf16),
            pltpu.VMEM((chunks, depth, value_cols), bf16),
            pltpu.VMEM((chunks, depth, key_cols), bf16),
            pltpu.VMEM((pairs, pair_rows, key_cols), f32),
            pltpu.VMEM((pairs, pair_rows, value_cols), f32),
            pltpu.VMEM((pairs, pair_rows, key_cols), f32),
            pltpu.VMEM((pairs, pair_rows, key_cols), f32),
            pltpu.VMEM((pairs, 1, key_cols), f32),
            pltpu.VMEM((heads, cue, dv), f32),
            pltpu.VMEM((1, lanes_padded), f32),
            pltpu.VMEM((n_sp, 1, lanes_padded), f32),
            pltpu.VMEM((n_sp, message, dv), f32),
            pltpu.VMEM((n_sp, message, dv), f32),
            dma((chunks,)),
            dma((3, chunks)),
            dma((pairs, chunks)),
            dma((pairs, chunks)),
            dma((pairs, chunks)),
            dma((pairs, chunks)),
            dma((n_sp,)),
            dma((n_sp,)),
            dma((n_sp,)),
            dma((n_sp,)),
        ],
        compiler_params=pltpu.CompilerParams(
            collective_id=0, has_side_effects=True, vmem_limit_bytes=60 * 1024 * 1024
        ),
        name="gated_state",
    )(
        tokens, lock_projector, value_weight, decay_weight,
        decay_offset.reshape(1, key_cols), fresh_question,
    )
    return pl.pallas_call(
        functools.partial(finish, heads, row_span),
        out_shape=(
            jax.ShapeDtypeStruct((heads, row_span, dv), bf16),
            jax.ShapeDtypeStruct((heads, dv), bf16),
        ),
        in_specs=[vmem_spec],
        out_specs=(vmem_spec, vmem_spec),
        name="finish",
    )(total)


def solution(mesh):
    in_specs = (
        P(("sp", "tp"), None),
        P(None, "tp"),
        P(None, "tp"),
        P(None, "tp"),
        P("tp"),
        P("tp", None),
    )
    out_specs = (P("tp", "sp", None), P("tp", None))
    body = functools.partial(per_device, mesh.shape["sp"], mesh.shape["tp"])
    return jax.shard_map(body, mesh=mesh, in_specs=in_specs, out_specs=out_specs, check_vma=False)
```

```python
import functools
import math

import jax
import jax.numpy as jnp
from jax import lax
from jax.experimental import pallas as pl
from jax.experimental.pallas import tpu as pltpu
from jax.sharding import PartitionSpec as P

DECAY_TAU = 16.0
CORES = 2
LANES = 128
MESH = pl.DeviceIdType.MESH


def kernel(
    n_sp, n_tp, chunks,
    tokens, w_key, w_value, w_decay, offset, question,
    total_out,
    x_buf, key_buf, value_buf, decay_buf, key_acc, value_acc, decay_acc,
    log_buf, pair_total, spread_q, total_send, total_recv, state_send, state_recv,
    token_sem, weight_sem, y_send, y_recv, d_send, d_recv, t_send, t_recv, s_send, s_recv,
):
    rows, width = tokens.shape
    key_cols = w_key.shape[1]
    heads, cue = question.shape
    dv = w_value.shape[1] // heads
    depth = width // chunks
    pairs = n_tp // CORES
    pair_rows = CORES * rows
    row_span = cue // n_sp
    lanes_padded = total_send.shape[-1]
    length = rows * n_tp * n_sp

    sp = lax.axis_index("sp")
    tp = lax.axis_index("tp")
    pair = tp // CORES
    core = lax.rem(tp, CORES)
    partner = pair * CORES + (1 - core)

    def pair_at(i):
        return lax.rem(pair + pairs - i, pairs)

    def token_copy(c):
        start = c * depth if isinstance(c, int) else pl.multiple_of(c * depth, depth)
        return pltpu.make_async_copy(
            tokens.at[:, pl.ds(start, depth)], x_buf.at[c, pair, core], token_sem.at[c]
        )

    def weight_copies(c):
        start = c * depth if isinstance(c, int) else pl.multiple_of(c * depth, depth)
        return [
            pltpu.make_async_copy(w.at[pl.ds(start, depth), :], b.at[c], weight_sem.at[n, c])
            for n, (w, b) in enumerate(
                ((w_decay, decay_buf), (w_key, key_buf), (w_value, value_buf))
            )
        ]

    def across_send(i, c):
        to = lax.rem(pair + i, pairs) * CORES + core
        block = x_buf.at[c, pair, core]
        return pltpu.make_async_remote_copy(
            block, block, y_send.at[i, c], y_recv.at[i, c], device_id={"tp": to}, device_id_type=MESH
        )

    def across_recv(i, c):
        block = x_buf.at[c, pair_at(i), core]
        return pltpu.make_async_remote_copy(
            block, block, y_send.at[i, c], y_recv.at[i, c],
            device_id={"tp": pair_at(i) * CORES + core}, device_id_type=MESH,
        )

    def beside(i, c, which):
        block = x_buf.at[c, pair_at(i), which]
        return pltpu.make_async_remote_copy(
            block, block, d_send.at[i, c], d_recv.at[i, c],
            device_id={"tp": partner}, device_id_type=MESH,
        )

    def total_copy(i, slot):
        return pltpu.make_async_remote_copy(
            total_send, total_recv.at[slot], t_send.at[i], t_recv.at[i],
            device_id={"sp": lax.rem(sp + i, n_sp)}, device_id_type=MESH,
        )

    def state_copy(i, slot):
        to = lax.rem(sp + i, n_sp)
        return pltpu.make_async_remote_copy(
            state_send.at[to], state_recv.at[slot], s_send.at[i], s_recv.at[i],
            device_id={"sp": to}, device_id_type=MESH,
        )

    for c in range(chunks):
        token_copy(c).start()
    for c in range(chunks):
        for copy in weight_copies(c):
            copy.start()

    barrier = pltpu.get_barrier_semaphore()
    pl.semaphore_signal(barrier, inc=1, device_id={"tp": partner}, device_id_type=MESH)
    for i in range(1, pairs):
        pl.semaphore_signal(
            barrier, inc=1,
            device_id={"tp": lax.rem(pair + i, pairs) * CORES + core}, device_id_type=MESH,
        )
    for i in range(1, n_sp):
        pl.semaphore_signal(
            barrier, inc=1, device_id={"sp": lax.rem(sp + i, n_sp)}, device_id_type=MESH
        )

    wide_q = question[...].astype(jnp.float32)
    eye = lax.broadcasted_iota(jnp.int32, (cue, cue), 0) == lax.broadcasted_iota(
        jnp.int32, (cue, cue), 1
    )
    ones = jnp.ones((cue, dv), jnp.bfloat16)
    for h in range(heads):
        diagonal = jnp.where(eye, jnp.broadcast_to(wide_q[h : h + 1, :], (cue, cue)), 0.0)
        spread_q[h] = jnp.dot(
            diagonal.astype(jnp.bfloat16), ones, preferred_element_type=jnp.float32
        )

    pl.semaphore_wait(barrier, 1 + (pairs - 1) + (n_sp - 1))

    for c in range(chunks):
        token_copy(c).wait()
        for i in range(1, pairs):
            across_send(i, c).start()
    for c in range(chunks):
        beside(0, c, core).start()

    def product(p, c, buf, acc, first):
        x = x_buf[c, p].reshape(pair_rows, depth)
        out = jnp.dot(x, buf[c], preferred_element_type=jnp.float32)
        if first:
            acc[p] = out
        else:
            acc[p] += out

    def all_products(p, c, first):
        product(p, c, decay_buf, decay_acc, first)
        product(p, c, key_buf, key_acc, first)
        product(p, c, value_buf, value_acc, first)

    def finish_decay(p):
        pre = decay_acc[p] + offset[...] + math.log(length)
        log_decay = (jnp.minimum(pre, 0.0) - jnp.log1p(jnp.exp(-jnp.abs(pre)))) / DECAY_TAU
        log_buf[p] = log_decay
        pair_total[p] = jnp.sum(log_decay, axis=0, keepdims=True)

    def send_totals():
        whole = pair_total[0]
        for p in range(1, pairs):
            whole = whole + pair_total[p]
        if lanes_padded > key_cols:
            whole = jnp.concatenate(
                [whole, jnp.zeros((1, lanes_padded - key_cols), jnp.float32)], axis=1
            )
        total_send[...] = whole
        total_recv[sp] = whole
        for i in range(1, n_sp):
            total_copy(i, sp).start()

    def arrive(i, c):
        if i == 0:
            for copy in weight_copies(c):
                copy.wait()
        else:
            across_recv(i, c).wait_recv()
            beside(i, c, core).start()

    for i in range(pairs):
        p = pair_at(i)
        arrive(i, 0)
        arrive(i, 1)
        beside(i, 0, 1 - core).wait_recv()
        all_products(p, 0, True)

        def step(c, carry, i=i, p=p):
            arrive(i, c + 1)
            beside(i, c, 1 - core).wait_recv()
            all_products(p, c, False)
            return carry

        lax.fori_loop(1, chunks - 1, step, 0)
        last = chunks - 1
        beside(i, last, 1 - core).wait_recv()
        product(p, last, decay_buf, decay_acc, False)
        finish_decay(p)
        if i == pairs - 1:
            send_totals()
        product(p, last, key_buf, key_acc, False)
        product(p, last, value_buf, value_acc, False)

    later = lax.broadcasted_iota(jnp.int32, (pair_rows, pair_rows), 1) > lax.broadcasted_iota(
        jnp.int32, (pair_rows, pair_rows), 0
    )
    later = jnp.where(later, 1.0, 0.0).astype(jnp.bfloat16)
    group = 2 if heads % 2 == 0 else 1
    gk, gv = group * cue, group * dv
    sums = [None] * (heads // group)
    behind = jnp.zeros((1, key_cols), jnp.float32)
    for p in reversed(range(pairs)):
        log_decay = log_buf[p]
        after = behind
        rest = log_decay
        for _ in range(3):
            part = rest.astype(jnp.bfloat16)
            rest = rest - part.astype(jnp.float32)
            after = after + jnp.dot(later, part, preferred_element_type=jnp.float32)
        behind = behind + pair_total[p]
        keys = key_acc[p].astype(jnp.bfloat16).astype(jnp.float32)
        exact = keys * jnp.exp(after)
        upper = exact.astype(jnp.bfloat16)
        lower = (exact - upper.astype(jnp.float32)).astype(jnp.bfloat16)
        values = value_acc[p].astype(jnp.bfloat16)
        for g in range(heads // group):
            for weighted in (upper, lower):
                term = lax.dot_general(
                    weighted[:, g * gk : (g + 1) * gk],
                    values[:, g * gv : (g + 1) * gv],
                    (((0,), (0,)), ((), ())),
                    preferred_element_type=jnp.float32,
                )
                sums[g] = term if sums[g] is None else sums[g] + term

    for i in range(1, n_sp):
        total_copy(i, lax.rem(sp + n_sp - i, n_sp)).wait_recv()
    later_total = jnp.zeros((1, lanes_padded), jnp.float32)
    for s in range(n_sp):
        later_total = later_total + jnp.where(sp < s, total_recv[s], 0.0)
    kept = jnp.exp(later_total)
    base = heads * row_span
    for g in range(heads // group):
        lo = g * gk // LANES * LANES
        turned = jnp.broadcast_to(kept[:, lo : lo + LANES], (LANES, LANES)).T
        for j in range(group):
            h = g * group + j
            at = h * cue - lo
            spread = turned[at : at + cue]
            if dv != LANES:
                spread = jnp.broadcast_to(spread[:, :1], (cue, dv))
            state = sums[g][j * cue : (j + 1) * cue, j * dv : (j + 1) * dv] * spread
            heard = jnp.sum(state * spread_q[h], axis=0, keepdims=True) * cue**-0.5
            for s in range(n_sp):
                state_send[s, h * row_span : (h + 1) * row_span, :] = state[
                    s * row_span : (s + 1) * row_span
                ]
                state_send[s, base + h : base + h + 1, :] = heard
    for i in range(1, n_sp):
        state_copy(i, sp).start()
    state_recv[sp] = state_send[sp]
    for i in range(1, n_sp):
        state_copy(i, lax.rem(sp + n_sp - i, n_sp)).wait_recv()
    total = state_recv[0]
    for s in range(1, n_sp):
        total = total + state_recv[s]
    total_out[...] = total

    def drain(c, carry):
        for i in range(1, pairs):
            across_send(i, c).wait_send()
        for i in range(pairs):
            beside(i, c, core).wait_send()
        return carry

    lax.fori_loop(0, chunks, drain, 0)
    for i in range(1, n_sp):
        total_copy(i, sp).wait_send()
        state_copy(i, sp).wait_send()


def finish(heads, row_span, total, cache_out, read_out):
    for h in range(heads):
        cache_out[h] = total[h * row_span : (h + 1) * row_span, :].astype(jnp.bfloat16)
    heard = total[heads * row_span : heads * (row_span + 1), :]
    scale = lax.rsqrt(jnp.mean(heard * heard, axis=-1, keepdims=True) + 1.0)
    read_out[...] = (heard * scale).astype(jnp.bfloat16)


def per_device(n_sp, n_tp, tokens, lock_projector, value_weight, decay_weight, decay_offset, fresh_question):
    rows, width = tokens.shape
    key_cols = lock_projector.shape[1]
    value_cols = value_weight.shape[1]
    heads, cue = fresh_question.shape
    dv = value_cols // heads
    row_span = cue // n_sp
    pairs = n_tp // CORES
    chunks = 4
    depth = width // chunks
    lanes_padded = max(key_cols, LANES)
    message = heads * row_span + heads
    f32, bf16 = jnp.float32, jnp.bfloat16
    dma = pltpu.SemaphoreType.DMA
    any_spec = pl.BlockSpec(memory_space=pl.ANY)
    vmem_spec = pl.BlockSpec(memory_space=pltpu.VMEM)
    pair_rows = CORES * rows
    total = pl.pallas_call(
        functools.partial(kernel, n_sp, n_tp, chunks),
        out_shape=jax.ShapeDtypeStruct((message, dv), f32),
        in_specs=[any_spec] * 4 + [vmem_spec] * 2,
        out_specs=vmem_spec,
        scratch_shapes=[
            pltpu.VMEM((chunks, pairs, CORES, rows, depth), bf16),
            pltpu.VMEM((chunks, depth, key_cols), bf16),
            pltpu.VMEM((chunks, depth, value_cols), bf16),
            pltpu.VMEM((chunks, depth, key_cols), bf16),
            pltpu.VMEM((pairs, pair_rows, key_cols), f32),
            pltpu.VMEM((pairs, pair_rows, value_cols), f32),
            pltpu.VMEM((pairs, pair_rows, key_cols), f32),
            pltpu.VMEM((pairs, pair_rows, key_cols), f32),
            pltpu.VMEM((pairs, 1, key_cols), f32),
            pltpu.VMEM((heads, cue, dv), f32),
            pltpu.VMEM((1, lanes_padded), f32),
            pltpu.VMEM((n_sp, 1, lanes_padded), f32),
            pltpu.VMEM((n_sp, message, dv), f32),
            pltpu.VMEM((n_sp, message, dv), f32),
            dma((chunks,)),
            dma((3, chunks)),
            dma((pairs, chunks)),
            dma((pairs, chunks)),
            dma((pairs, chunks)),
            dma((pairs, chunks)),
            dma((n_sp,)),
            dma((n_sp,)),
            dma((n_sp,)),
            dma((n_sp,)),
        ],
        compiler_params=pltpu.CompilerParams(
            collective_id=0, has_side_effects=True, vmem_limit_bytes=60 * 1024 * 1024
        ),
        name="gated_state",
    )(
        tokens, lock_projector, value_weight, decay_weight,
        decay_offset.reshape(1, key_cols), fresh_question,
    )
    return pl.pallas_call(
        functools.partial(finish, heads, row_span),
        out_shape=(
            jax.ShapeDtypeStruct((heads, row_span, dv), bf16),
            jax.ShapeDtypeStruct((heads, dv), bf16),
        ),
        in_specs=[vmem_spec],
        out_specs=(vmem_spec, vmem_spec),
        name="finish",
    )(total)


def solution(mesh):
    in_specs = (
        P(("sp", "tp"), None),
        P(None, "tp"),
        P(None, "tp"),
        P(None, "tp"),
        P("tp"),
        P("tp", None),
    )
    out_specs = (P("tp", "sp", None), P("tp", None))
    body = functools.partial(per_device, mesh.shape["sp"], mesh.shape["tp"])
    return jax.shard_map(body, mesh=mesh, in_specs=in_specs, out_specs=out_specs, check_vma=False)
```
